32 devices in a mesh: sp: 8 (over z, y), tp: 4 (over x, core).
Axes of the slice: x: 2, y: 2, z: 4, core: 2. Of those that a mesh axis runs over, the one named last changes fastest.
Arguments:
- queries: bfloat16 [6144, 2048], P('sp', 'tp'), may hold values from -11 to 11
- key_rows: bfloat16 [6144, 2048], P('sp', 'tp'), may hold values from -4.5 to 4.5
- value_rows: bfloat16 [6144, 2048], P('sp', 'tp'), may hold values from -6 to 6
- log_forget: float32 [6144, 32], P('sp', 'tp'), may hold values from -740.28 to 0, as said below
- stream_in: bfloat16 [6144, 2048], P('sp'), may hold values from -6 to 6
- out_weight: bfloat16 [2048, 2048], P('tp'), may hold values from -0.52734375 to 0.52734375
- mix_gain: float32 [2048], replicated, may hold values from 0.1 to 1.9
- mix_bias: float32 [2048], replicated, may hold values from -3 to 3
- gate_weight: bfloat16 [2048, 5632], P('sp', 'tp'), may hold values from -0.125 to 0.125
- up_weight: bfloat16 [2048, 5632], P('sp', 'tp'), may hold values from -0.125 to 0.125
- down_weight: bfloat16 [5632, 2048], P('tp', 'sp'), may hold values from -0.15917969 to 0.15917969
- ffn_gain: float32 [2048], replicated, may hold values from 0.1 to 1.9
- ffn_bias: float32 [2048], replicated, may hold values from -3 to 3
Outputs:
- layer_out: bfloat16 [6144, 2048], P(('sp', 'tp'))
The draws below stay inside these ranges and needn't reach their ends.
Inputs may be any that keep to these rules, and one draw needn't show every extreme that they name: `log_forget`: each column never rises along the positions.
All inputs are finite; a program needn't handle non-finite values.
Results may differ from the reference program's by a relative error of at most 0.015.
Values may be sent and summed in bfloat16 or wider, within the bound.
A program may use at most 128 MiB of HBM per device.

```python
import math
import jax
import jax.numpy as jnp
from jax import lax

D = 2048
HEAD_TOTAL = 32
FF = 5632
TOK_DEV = 768
SEQUENCE_LENGTH = 6144
N_SP = 8


def draw_queries(key, part):
    base_noise = jax.random.normal(jax.random.fold_in(key, 1), (SEQUENCE_LENGTH, D), jnp.float32)
    row_scale = jnp.exp(jax.random.uniform(jax.random.fold_in(key, 31), (SEQUENCE_LENGTH, 1), jnp.float32, -0.7, 1.6))
    base_noise = jnp.clip(base_noise * row_scale, -11.0, 11.0)
    return base_noise.astype(jnp.bfloat16)


def draw_key_rows(key, part):
    base_noise = jax.random.normal(jax.random.fold_in(key, 2), (SEQUENCE_LENGTH, D), jnp.float32)
    row_scale = jnp.exp(jax.random.uniform(jax.random.fold_in(key, 32), (SEQUENCE_LENGTH, 1), jnp.float32, -0.8, 0.8))
    base_noise = jnp.clip(base_noise * row_scale, -4.5, 4.5)
    return base_noise.astype(jnp.bfloat16)


def draw_log_forget(key, part):
    head_order = jax.random.permutation(jax.random.fold_in(key, 21), HEAD_TOTAL)
    sluggish_heads = head_order < HEAD_TOTAL // 2
    fast_rate = jnp.exp(jax.random.uniform(jax.random.fold_in(key, 22), (HEAD_TOTAL,), jnp.float32, math.log(1.0 / 100.0), math.log(1.0 / 30.0)))
    head_rate = jnp.where(sluggish_heads, 0.5 / SEQUENCE_LENGTH, fast_rate)
    block_count = SEQUENCE_LENGTH // TOK_DEV
    block_factor = jnp.exp(jax.random.uniform(jax.random.fold_in(key, 23), (block_count, HEAD_TOTAL), jnp.float32, math.log(0.5), math.log(2.0)))
    position_factor = jax.random.uniform(jax.random.fold_in(key, 24), (SEQUENCE_LENGTH, HEAD_TOTAL), jnp.float32, 0.25, 1.75)
    logarithm_increments = -head_rate[None, :] * jnp.repeat(block_factor, TOK_DEV, axis=0) * position_factor
    spike_locations = jax.random.randint(jax.random.fold_in(key, 25), (3, HEAD_TOTAL), 0, SEQUENCE_LENGTH)
    spike_lengths = jax.random.uniform(jax.random.fold_in(key, 26), (3, HEAD_TOTAL), jnp.float32, 0.22, 0.69)
    token_positions = jnp.arange(SEQUENCE_LENGTH, dtype=jnp.int32)
    for spike_index in range(3):
        spike_matches = (token_positions[:, None] == spike_locations[spike_index][None, :]) & sluggish_heads[None, :]
        logarithm_increments = logarithm_increments - jnp.where(spike_matches, spike_lengths[spike_index][None, :], 0.0)
    return jnp.cumsum(logarithm_increments, axis=0).astype(jnp.float32)


def levels(key, dims, cuts, low, largest):
    level, own = 1.0, jax.random.fold_in(key, 6)
    for axis_at, blocks in cuts:
        heights = jnp.exp(jax.random.uniform(jax.random.fold_in(own, axis_at), (blocks,), jnp.float32, low / len(cuts), largest / len(cuts)))
        level = level * jnp.repeat(heights, dims[axis_at] // blocks).reshape([-1 if axis == axis_at else 1 for axis in range(len(dims))])
    return level


def scatter_about(key, extent, width, most, split=(), kind=jnp.bfloat16):
    values = width * jax.random.normal(key, extent, jnp.float32)
    if split:
        values = values * levels(key, extent, split, -0.22, 0.18)
    return jnp.clip(values, -most, most).astype(kind)


def setup_inputs(seed: int = 0) -> dict:
    seeds = jax.random.split(jax.random.key(seed), 14)
    return {
        "queries": draw_queries(jax.random.fold_in(seeds[13], 71), 0),
        "key_rows": draw_key_rows(jax.random.fold_in(seeds[13], 71), 0),
        "value_rows": scatter_about(seeds[2], (SEQUENCE_LENGTH, D), 1.0, 6.0, ((0, 8), (1, 4))),
        "log_forget": draw_log_forget(jax.random.fold_in(seeds[13], 71), 0),
        "stream_in": scatter_about(seeds[4], (SEQUENCE_LENGTH, D), 1.0, 6.0, ((0, 8),)),
        "out_weight": scatter_about(seeds[5], (D, D), (4.0 * D ** -0.5), 0.52734375, ((0, 4),)),
        "mix_gain": jnp.clip(1.0 + 0.18 * jax.random.normal(seeds[6], (D,), jnp.float32), 0.1, 1.9),
        "mix_bias": scatter_about(seeds[7], (D,), 0.5, 3.0, (), jnp.float32),
        "gate_weight": scatter_about(seeds[8], (D, FF), D ** -0.5, 0.125, ((0, 8), (1, 4))),
        "up_weight": scatter_about(seeds[9], (D, FF), D ** -0.5, 0.125, ((0, 8), (1, 4))),
        "down_weight": scatter_about(seeds[10], (FF, D), (2.0 * FF ** -0.5), 0.15917969, ((0, 4), (1, 8))),
        "ffn_gain": jnp.clip(1.0 + 0.18 * jax.random.normal(seeds[11], (D,), jnp.float32), 0.1, 1.9),
        "ffn_bias": scatter_about(seeds[12], (D,), 0.5, 3.0, (), jnp.float32),
    }


ALPHA = 8.0 ** 0.25
EPSILON = 1e-05

def layer_norm(matrix, norm_gain, norm_shift):
    centred = matrix - lax.optimization_barrier(jnp.mean(matrix, axis=-1, keepdims=True))
    spread = lax.optimization_barrier(jnp.mean(centred * centred, axis=-1, keepdims=True))
    return centred * lax.rsqrt(spread + EPSILON) * norm_gain + norm_shift

def head_attention(query_head, key_head, value_head, gate_head):
    head_dim = query_head.shape[1]
    score_scale = head_dim ** (-0.5)
    key_pos = jnp.arange(SEQUENCE_LENGTH, dtype=jnp.int32)
    query_blocks = query_head.reshape(N_SP, TOK_DEV, head_dim)
    gate_blocks = gate_head.reshape(N_SP, TOK_DEV)

    def one_block(packed):
        query_block, gate_block, block_index = packed
        scores = jnp.dot(query_block, key_head.T, preferred_element_type=jnp.float32) * score_scale
        scores = scores + gate_block[:, None] - gate_head[None, :]
        query_pos = block_index * TOK_DEV + jnp.arange(TOK_DEV, dtype=jnp.int32)
        allowed = key_pos[None, :] <= query_pos[:, None]
        masked = jnp.where(allowed, scores, -1e+30)
        highest = lax.optimization_barrier(jnp.max(masked, axis=1, keepdims=True))
        exponent = jnp.where(allowed, jnp.exp(masked - highest), 0.0)
        totals = lax.optimization_barrier(jnp.sum(exponent, axis=1, keepdims=True))
        weighted = jnp.dot(exponent.astype(jnp.bfloat16), value_head, preferred_element_type=jnp.float32)
        return (weighted / totals).astype(jnp.bfloat16)
    return lax.map(one_block, (query_blocks, gate_blocks, jnp.arange(N_SP, dtype=jnp.int32)))

def reference(queries, key_rows, value_rows, log_forget, stream_in, out_weight, mix_gain, mix_bias, gate_weight, up_weight, down_weight, ffn_gain, ffn_bias):
    head_count = log_forget.shape[1]
    head_dim = queries.shape[1] // head_count

    def split_heads(matrix):
        return matrix.reshape(SEQUENCE_LENGTH, head_count, head_dim).transpose(1, 0, 2)

    def per_head(packed):
        return head_attention(packed[0], packed[1], packed[2], packed[3])
    attended = lax.map(per_head, (split_heads(queries), split_heads(key_rows), split_heads(value_rows), log_forget.T))
    attended = attended.reshape(head_count, SEQUENCE_LENGTH, head_dim).transpose(1, 0, 2).reshape(SEQUENCE_LENGTH, head_count * head_dim)
    mix_out = jnp.dot(attended, out_weight, preferred_element_type=jnp.float32).astype(jnp.bfloat16)
    mix_out = lax.optimization_barrier(mix_out).astype(jnp.float32)
    normed = layer_norm(ALPHA * stream_in.astype(jnp.float32) + mix_out, mix_gain, mix_bias).astype(jnp.bfloat16)
    gate_part = jnp.dot(normed, gate_weight, preferred_element_type=jnp.float32)
    up_part = jnp.dot(normed, up_weight, preferred_element_type=jnp.float32)
    hidden = (jax.nn.silu(gate_part) * up_part).astype(jnp.bfloat16)
    lowered = jnp.dot(hidden, down_weight, preferred_element_type=jnp.float32).astype(jnp.bfloat16)
    lowered = lax.optimization_barrier(lowered).astype(jnp.float32)
    result = layer_norm(ALPHA * normed.astype(jnp.float32) + lowered, ffn_gain, ffn_bias)
    return result.astype(jnp.bfloat16)
```

```python
import jax
import jax.numpy as jnp
from jax import lax
from jax.experimental import pallas as pl
from jax.experimental.pallas import tpu as pltpu
from jax.sharding import PartitionSpec as P

ALPHA = 8.0**0.25
EPSILON = 1e-05


def layer_norm(matrix, norm_gain, norm_shift):
    centred = matrix - jnp.mean(matrix, axis=-1, keepdims=True)
    spread = jnp.mean(centred * centred, axis=-1, keepdims=True)
    return centred * lax.rsqrt(spread + EPSILON) * norm_gain + norm_shift


def attend(queries, key_rows, value_rows, log_forget):
    length, row_width = queries.shape
    head_count = log_forget.shape[1]
    head_dim = row_width // head_count
    score_scale = head_dim ** (-0.5)
    first_pos = lax.axis_index("sp") * length
    last_pos = first_pos + length
    query_heads = queries.reshape(length, head_count, head_dim)
    query_gates = log_forget.T
    query_pos = first_pos + jnp.arange(length, dtype=jnp.int32)
    gates_all = lax.all_gather(log_forget, "sp", axis=0, tiled=True)
    initial = (
        jnp.full((head_count, length), -1e30, jnp.float32),
        jnp.zeros((head_count, length), jnp.float32),
        jnp.zeros((length, head_count, head_dim), jnp.float32),
    )
    running = initial
    key_piece = lax.all_gather(key_rows, "sp", axis=0, tiled=True)
    value_piece = lax.all_gather(value_rows, "sp", axis=0, tiled=True)
    piece_len = key_piece.shape[0]
    shards = piece_len // length
    group_size = max(
        [
            count_try
            for count_try in range(1, shards + 1)
            if shards % count_try == 0 and count_try * length <= max(length, 512)
        ]
    )
    block_len = group_size * length
    blocks = piece_len // block_len
    key_blocks = key_piece.reshape(blocks, block_len, head_count, head_dim)
    value_blocks = value_piece.reshape(blocks, block_len, head_count, head_dim)
    gate_blocks = gates_all.reshape(blocks, block_len, head_count)
    block_starts = block_len * jnp.arange(blocks, dtype=jnp.int32)

    def one_block(running_state, packed):
        key_block, value_block, gate_block, block_start = packed

        def compute(state_in):
            highest, totals, weighted = state_in
            scores = (
                jnp.einsum(
                    "qhd,khd->hqk", query_heads, key_block, preferred_element_type=jnp.float32
                )
                * score_scale
            )
            scores = scores + query_gates[:, :, None] - gate_block.T[:, None, :]
            key_pos = block_start + jnp.arange(block_len, dtype=jnp.int32)
            allowed = (key_pos[None, :] <= query_pos[:, None])[None]
            masked = jnp.where(allowed, scores, -1e30)
            new_high = jnp.maximum(highest, jnp.max(masked, axis=2))
            weights = jnp.where(allowed, jnp.exp(masked - new_high[:, :, None]), 0.0)
            factor = jnp.exp(highest - new_high)
            totals = totals * factor + jnp.sum(weights, axis=2)
            weighted = weighted * factor.T[:, :, None] + jnp.einsum(
                "hqk,khd->qhd",
                weights.astype(jnp.bfloat16),
                value_block,
                preferred_element_type=jnp.float32,
            )
            return (new_high, totals, weighted)

        def keep_state(state_in):
            return state_in

        return (lax.cond(block_start < last_pos, compute, keep_state, running_state), None)

    running, unused = lax.scan(
        one_block, running, (key_blocks, value_blocks, gate_blocks, block_starts)
    )
    highest, totals, weighted = running
    return (weighted / totals.T[:, :, None]).reshape(length, row_width).astype(jnp.bfloat16)


SUB = 256


def flash_kernel(packed_ref, out_ref, query_ref, value_ref, high_ref, acc_ref):
    pieces, rows, length = packed_ref.shape
    head_dim = out_ref.shape[1]
    sub = SUB if length % SUB == 0 else length
    gate_rows = rows - 3 * head_dim
    query_at = head_dim + gate_rows
    value_at = query_at + head_dim
    tail = jnp.zeros((128 - head_dim - gate_rows, length), jnp.bfloat16)
    row_index = lax.broadcasted_iota(jnp.int32, (gate_rows, length), 0)
    minus = jnp.where(row_index < 3, -1.0, 0.0).astype(jnp.bfloat16)
    ones = jnp.where(row_index < 1, 1.0, 0.0).astype(jnp.bfloat16)
    scale = head_dim**-0.5

    def set_values(piece, carry):
        block = packed_ref[piece, value_at : value_at + head_dim, :]
        value_ref[piece] = jnp.concatenate([block, ones, tail], axis=0).T
        return carry

    lax.fori_loop(0, pieces, set_values, 0)

    def pair(piece, diagonal):
        key_block = packed_ref[piece, 0:128, :]
        for start in range(0, length, sub):
            width = min(length, start + sub) if diagonal else length
            keys = key_block[:, :width]
            scores = jnp.dot(
                query_ref[start : start + sub, :], keys, preferred_element_type=jnp.float32
            )
            if diagonal:
                key_pos = lax.broadcasted_iota(jnp.int32, (sub, width), 1)
                query_pos = start + lax.broadcasted_iota(jnp.int32, (sub, width), 0)
                scores = jnp.where(key_pos <= query_pos, scores, -1e30)
            old_high = high_ref[start : start + sub, :]
            new_high = jnp.maximum(old_high, jnp.max(scores, axis=1, keepdims=True))
            weights = jnp.exp(scores - new_high[:, :1]).astype(jnp.bfloat16)
            factor = jnp.exp(old_high - new_high)
            high_ref[start : start + sub, :] = new_high
            acc_ref[start : start + sub, :] = acc_ref[start : start + sub, :] * factor + jnp.dot(
                weights, value_ref[piece, :width, :], preferred_element_type=jnp.float32
            )

    def one_query_piece(index, carry):
        block = packed_ref[index, query_at : query_at + head_dim, :]
        scaled = (block.astype(jnp.float32) * scale).astype(jnp.bfloat16)
        query_ref[...] = jnp.concatenate([scaled, minus, tail], axis=0).T
        high_ref[...] = jnp.full_like(high_ref, -1e30)
        acc_ref[...] = jnp.zeros_like(acc_ref)

        def earlier(piece, inner):
            pair(piece, False)
            return inner

        lax.fori_loop(0, index, earlier, 0)
        pair(index, True)
        turned = acc_ref[...].T
        out_ref[index] = (turned[:head_dim] / turned[head_dim : head_dim + 1]).astype(jnp.bfloat16)
        return carry

    lax.fori_loop(0, pieces, one_query_piece, 0)


def attend_by_head(queries, key_rows, value_rows, log_forget):
    length, row_width = queries.shape
    heads = log_forget.shape[1]
    head_dim = row_width // heads
    pieces = lax.axis_size("sp")

    def turn(matrix):
        return matrix.T.reshape(heads, head_dim, length)

    gates = log_forget.T
    high = lax.reduce_precision(gates, 8, 7)
    middle = lax.reduce_precision(gates - high, 8, 7)
    low = gates - high - middle
    gate_rows = jnp.stack([high, middle, low], axis=1).astype(jnp.bfloat16)
    gate_rows = jnp.pad(gate_rows, ((0, 0), (0, 13), (0, 0)))
    packed = jnp.concatenate(
        [turn(key_rows), gate_rows, turn(queries), turn(value_rows)], axis=1
    )
    packed = lax.all_to_all(packed, "sp", 0, 0, tiled=True)
    flops = 2 * pieces * pieces * length * length * 128
    attended = pl.pallas_call(
        flash_kernel,
        out_shape=jax.ShapeDtypeStruct((pieces, head_dim, length), jnp.bfloat16),
        in_specs=[pl.BlockSpec(memory_space=pltpu.VMEM)],
        out_specs=pl.BlockSpec(memory_space=pltpu.VMEM),
        scratch_shapes=[
            pltpu.VMEM((length, 128), jnp.bfloat16),
            pltpu.VMEM((pieces, length, 128), jnp.bfloat16),
            pltpu.VMEM((length, 128), jnp.float32),
            pltpu.VMEM((length, 128), jnp.float32),
        ],
        compiler_params=pltpu.CompilerParams(vmem_limit_bytes=40 * 1024 * 1024),
        cost_estimate=pl.CostEstimate(
            flops=4 * flops, bytes_accessed=packed.size * 2, transcendentals=0
        ),
    )(packed)
    back = lax.all_to_all(attended, "sp", 0, 0, tiled=True)
    return back.reshape(row_width, length)


def body(
    queries,
    key_rows,
    value_rows,
    log_forget,
    stream_in,
    out_weight,
    mix_gain,
    mix_bias,
    gate_weight,
    up_weight,
    down_weight,
    ffn_gain,
    ffn_bias,
):
    length = queries.shape[0]
    heads = log_forget.shape[1]
    head_dim = queries.shape[1] // heads
    by_head = heads == lax.axis_size("sp") and head_dim + 16 <= 128 and head_dim % 16 == 0
    if by_head:
        turned = attend_by_head(queries, key_rows, value_rows, log_forget)
    else:
        turned = attend(queries, key_rows, value_rows, log_forget).T
    own_rows = length // lax.axis_size("tp")
    offset = lax.axis_index("tp") * own_rows
    summed = lax.psum_scatter(
        lax.dot_general(
            turned,
            out_weight,
            (((0,), (0,)), ((), ())),
            preferred_element_type=jnp.float32,
        ).astype(jnp.bfloat16),
        "tp",
        scatter_dimension=0,
        tiled=True,
    )
    mix_out = lax.optimization_barrier(summed).astype(jnp.float32)
    stream_own = lax.dynamic_slice_in_dim(stream_in, offset, own_rows, 0)
    normed = layer_norm(
        ALPHA * stream_own.astype(jnp.float32) + mix_out, mix_gain, mix_bias
    ).astype(jnp.bfloat16)
    gathered = lax.all_gather(normed, "tp", axis=0, tiled=True)
    gate_part = jnp.dot(
        gathered,
        lax.all_gather(gate_weight, "sp", axis=0, tiled=True),
        preferred_element_type=jnp.float32,
    )
    up_part = jnp.dot(
        gathered,
        lax.all_gather(up_weight, "sp", axis=0, tiled=True),
        preferred_element_type=jnp.float32,
    )
    hidden = (jax.nn.silu(gate_part) * up_part).astype(jnp.bfloat16)
    partial_terms = jnp.dot(
        hidden,
        lax.all_gather(down_weight, "sp", axis=1, tiled=True),
        preferred_element_type=jnp.float32,
    )
    lowered = lax.psum_scatter(
        partial_terms.astype(jnp.bfloat16), "tp", scatter_dimension=0, tiled=True
    ).astype(jnp.float32)
    lowered = lax.optimization_barrier(lowered.astype(jnp.bfloat16)).astype(jnp.float32)
    result = layer_norm(ALPHA * normed.astype(jnp.float32) + lowered, ffn_gain, ffn_bias)
    return result.astype(jnp.bfloat16)


def solution(mesh):
    placed = (
        P("sp", "tp"),
        P("sp", "tp"),
        P("sp", "tp"),
        P("sp", "tp"),
        P("sp", None),
        P("tp", None),
        P(),
        P(),
        P("sp", "tp"),
        P("sp", "tp"),
        P("tp", "sp"),
        P(),
        P(),
    )
    return jax.shard_map(
        body, mesh=mesh, in_specs=placed, out_specs=P(("sp", "tp"), None), check_vma=False
    )
```

```python
import jax
import jax.numpy as jnp
from jax import lax
from jax.experimental import pallas as pl
from jax.experimental.pallas import tpu as pltpu
from jax.sharding import PartitionSpec as P


ALPHA = 8.0**0.25
EPSILON = 1e-05


def layer_norm(matrix, norm_gain, norm_shift):
    centred = matrix - jnp.mean(matrix, axis=-1, keepdims=True)
    spread = jnp.mean(centred * centred, axis=-1, keepdims=True)
    return centred * lax.rsqrt(spread + EPSILON) * norm_gain + norm_shift


def attend(queries, key_rows, value_rows, log_forget):
    length, row_width = queries.shape
    head_count = log_forget.shape[1]
    head_dim = row_width // head_count
    score_scale = head_dim ** (-0.5)
    first_pos = lax.axis_index("sp") * length
    last_pos = first_pos + length
    query_heads = queries.reshape(length, head_count, head_dim)
    query_gates = log_forget.T
    query_pos = first_pos + jnp.arange(length, dtype=jnp.int32)
    gates_all = lax.all_gather(log_forget, "sp", axis=0, tiled=True)
    initial = (
        jnp.full((head_count, length), -1e30, jnp.float32),
        jnp.zeros((head_count, length), jnp.float32),
        jnp.zeros((length, head_count, head_dim), jnp.float32),
    )
    running = initial
    key_piece = lax.all_gather(key_rows, "sp", axis=0, tiled=True)
    value_piece = lax.all_gather(value_rows, "sp", axis=0, tiled=True)
    piece_len = key_piece.shape[0]
    shards = piece_len // length
    group_size = max(
        [
            count_try
            for count_try in range(1, shards + 1)
            if shards % count_try == 0 and count_try * length <= max(length, 512)
        ]
    )
    block_len = group_size * length
    blocks = piece_len // block_len
    key_blocks = key_piece.reshape(blocks, block_len, head_count, head_dim)
    value_blocks = value_piece.reshape(blocks, block_len, head_count, head_dim)
    gate_blocks = gates_all.reshape(blocks, block_len, head_count)
    block_starts = block_len * jnp.arange(blocks, dtype=jnp.int32)

    def one_block(running_state, packed):
        key_block, value_block, gate_block, block_start = packed

        def compute(state_in):
            highest, totals, weighted = state_in
            scores = (
                jnp.einsum(
                    "qhd,khd->hqk", query_heads, key_block, preferred_element_type=jnp.float32
                )
                * score_scale
            )
            scores = scores + query_gates[:, :, None] - gate_block.T[:, None, :]
            key_pos = block_start + jnp.arange(block_len, dtype=jnp.int32)
            allowed = (key_pos[None, :] <= query_pos[:, None])[None]
            masked = jnp.where(allowed, scores, -1e30)
            new_high = jnp.maximum(highest, jnp.max(masked, axis=2))
            weights = jnp.where(allowed, jnp.exp(masked - new_high[:, :, None]), 0.0)
            factor = jnp.exp(highest - new_high)
            totals = totals * factor + jnp.sum(weights, axis=2)
            weighted = weighted * factor.T[:, :, None] + jnp.einsum(
                "hqk,khd->qhd",
                weights.astype(jnp.bfloat16),
                value_block,
                preferred_element_type=jnp.float32,
            )
            return (new_high, totals, weighted)

        def keep_state(state_in):
            return state_in

        return (lax.cond(block_start < last_pos, compute, keep_state, running_state), None)

    running, unused = lax.scan(
        one_block, running, (key_blocks, value_blocks, gate_blocks, block_starts)
    )
    highest, totals, weighted = running
    return (weighted / totals.T[:, :, None]).reshape(length, row_width).astype(jnp.bfloat16)


SUB = 256


def flash_kernel(packed_ref, out_ref, query_ref, value_ref, high_ref, acc_ref):
    pieces, rows, length = packed_ref.shape
    head_dim = out_ref.shape[1]
    sub = SUB if length % SUB == 0 else length
    gate_rows = rows - 3 * head_dim
    query_at = head_dim + gate_rows
    value_at = query_at + head_dim
    tail = jnp.zeros((128 - head_dim - gate_rows, length), jnp.bfloat16)
    row_index = lax.broadcasted_iota(jnp.int32, (gate_rows, length), 0)
    minus = jnp.where(row_index < 3, -1.0, 0.0).astype(jnp.bfloat16)
    ones = jnp.where(row_index < 1, 1.0, 0.0).astype(jnp.bfloat16)
    scale = head_dim**-0.5

    def set_values(piece, carry):
        block = packed_ref[piece, value_at : value_at + head_dim, :]
        value_ref[piece] = jnp.concatenate([block, ones, tail], axis=0).T
        return carry

    lax.fori_loop(0, pieces, set_values, 0)

    def pair(piece, diagonal):
        key_block = packed_ref[piece, 0:128, :]
        for start in range(0, length, sub):
            width = min(length, start + sub) if diagonal else length
            keys = key_block[:, :width]
            scores = jnp.dot(
                query_ref[start : start + sub, :], keys, preferred_element_type=jnp.float32
            )
            if diagonal:
                key_pos = lax.broadcasted_iota(jnp.int32, (sub, width), 1)
                query_pos = start + lax.broadcasted_iota(jnp.int32, (sub, width), 0)
                scores = jnp.where(key_pos <= query_pos, scores, -1e30)
            old_high = high_ref[start : start + sub, :]
            new_high = jnp.maximum(old_high, jnp.max(scores, axis=1, keepdims=True))
            weights = jnp.exp(scores - new_high[:, :1]).astype(jnp.bfloat16)
            factor = jnp.exp(old_high - new_high)
            high_ref[start : start + sub, :] = new_high
            acc_ref[start : start + sub, :] = acc_ref[start : start + sub, :] * factor + jnp.dot(
                weights, value_ref[piece, :width, :], preferred_element_type=jnp.float32
            )

    def one_query_piece(index, carry):
        block = packed_ref[index, query_at : query_at + head_dim, :]
        scaled = (block.astype(jnp.float32) * scale).astype(jnp.bfloat16)
        query_ref[...] = jnp.concatenate([scaled, minus, tail], axis=0).T
        high_ref[...] = jnp.full_like(high_ref, -1e30)
        acc_ref[...] = jnp.zeros_like(acc_ref)

        def earlier(piece, inner):
            pair(piece, False)
            return inner

        lax.fori_loop(0, index, earlier, 0)
        pair(index, True)
        turned = acc_ref[...].T
        out_ref[index] = (turned[:head_dim] / turned[head_dim : head_dim + 1]).astype(jnp.bfloat16)
        return carry

    lax.fori_loop(0, pieces, one_query_piece, 0)


def attend_by_head(queries, key_rows, value_rows, log_forget):
    length, row_width = queries.shape
    heads = log_forget.shape[1]
    head_dim = row_width // heads
    pieces = lax.axis_size("sp")

    def turn(matrix):
        return matrix.T.reshape(heads, head_dim, length)

    gates = log_forget.T
    high = lax.reduce_precision(gates, 8, 7)
    middle = lax.reduce_precision(gates - high, 8, 7)
    low = gates - high - middle
    gate_rows = jnp.stack([high, middle, low], axis=1).astype(jnp.bfloat16)
    gate_rows = jnp.pad(gate_rows, ((0, 0), (0, 13), (0, 0)))
    packed = jnp.concatenate(
        [turn(key_rows), gate_rows, turn(queries), turn(value_rows)], axis=1
    )
    packed = lax.all_to_all(packed, "sp", 0, 0, tiled=True)
    flops = 2 * pieces * pieces * length * length * 128
    attended = pl.pallas_call(
        flash_kernel,
        out_shape=jax.ShapeDtypeStruct((pieces, head_dim, length), jnp.bfloat16),
        in_specs=[pl.BlockSpec(memory_space=pltpu.VMEM)],
        out_specs=pl.BlockSpec(memory_space=pltpu.VMEM),
        scratch_shapes=[
            pltpu.VMEM((length, 128), jnp.bfloat16),
            pltpu.VMEM((pieces, length, 128), jnp.bfloat16),
            pltpu.VMEM((length, 128), jnp.float32),
            pltpu.VMEM((length, 128), jnp.float32),
        ],
        compiler_params=pltpu.CompilerParams(vmem_limit_bytes=40 * 1024 * 1024),
        cost_estimate=pl.CostEstimate(
            flops=4 * flops, bytes_accessed=packed.size * 2, transcendentals=0
        ),
    )(packed)
    back = lax.all_to_all(attended, "sp", 0, 0, tiled=True)
    return back.reshape(row_width, length)


def swap_cores(block):
    count = lax.axis_size("tp")
    return lax.ppermute(block, "tp", [(i, i ^ 1) for i in range(count)])


def swap_across(block):
    count = lax.axis_size("tp")
    return lax.ppermute(block, "tp", [(i, i ^ 2) for i in range(count)])


def body(
    queries,
    key_rows,
    value_rows,
    log_forget,
    stream_in,
    out_weight,
    mix_gain,
    mix_bias,
    gate_weight,
    up_weight,
    down_weight,
    ffn_gain,
    ffn_bias,
):
    gate_full = lax.all_gather(gate_weight, "sp", axis=0, tiled=True)
    up_full = lax.all_gather(up_weight, "sp", axis=0, tiled=True)
    down_full = lax.all_gather(down_weight, "sp", axis=1, tiled=True)
    length = queries.shape[0]
    heads = log_forget.shape[1]
    head_dim = queries.shape[1] // heads
    by_head = heads == lax.axis_size("sp") and head_dim + 16 <= 128 and head_dim % 16 == 0
    if by_head:
        turned = attend_by_head(queries, key_rows, value_rows, log_forget)
    else:
        turned = attend(queries, key_rows, value_rows, log_forget).T
    own_rows = length // lax.axis_size("tp")
    offset = lax.axis_index("tp") * own_rows
    two_level = lax.axis_size("tp") == 4
    partial_mix = lax.dot_general(
        turned, out_weight, (((0,), (0,)), ((), ())), preferred_element_type=jnp.float32
    ).astype(jnp.bfloat16)
    if two_level:
        core = lax.axis_index("tp") % 2
        across = lax.axis_index("tp") // 2
        split = partial_mix.reshape(2, 2, own_rows, -1)
        mine = lax.dynamic_index_in_dim(split, core, 1, keepdims=False)
        other = lax.dynamic_index_in_dim(split, 1 - core, 1, keepdims=False)
        both = mine.astype(jnp.float32) + swap_cores(other).astype(jnp.float32)
        own = lax.dynamic_index_in_dim(both, across, 0, keepdims=False)
        away = lax.dynamic_index_in_dim(both, 1 - across, 0, keepdims=False)
        summed = (own + swap_across(away.astype(jnp.bfloat16)).astype(jnp.float32)).astype(
            jnp.bfloat16
        )
    else:
        summed = lax.psum_scatter(partial_mix, "tp", scatter_dimension=0, tiled=True)
    mix_out = lax.optimization_barrier(summed).astype(jnp.float32)
    stream_own = lax.dynamic_slice_in_dim(stream_in, offset, own_rows, 0)
    normed = layer_norm(
        ALPHA * stream_own.astype(jnp.float32) + mix_out, mix_gain, mix_bias
    ).astype(jnp.bfloat16)
    if two_level:
        pair = jnp.concatenate([normed, swap_across(normed)], axis=0)
        gathered = jnp.concatenate([pair, swap_cores(pair)], axis=0)
    else:
        gathered = lax.all_gather(normed, "tp", axis=0, tiled=True)
    gate_part = jnp.dot(gathered, gate_full, preferred_element_type=jnp.float32)
    up_part = jnp.dot(gathered, up_full, preferred_element_type=jnp.float32)
    hidden = (jax.nn.silu(gate_part) * up_part).astype(jnp.bfloat16)
    if two_level:
        columns = []
        half = down_full.shape[1] // 2
        for start in (0, half):
            terms = jnp.dot(
                hidden, down_full[:, start : start + half], preferred_element_type=jnp.float32
            ).astype(jnp.bfloat16)
            both = terms[: 2 * own_rows].astype(jnp.float32) + swap_cores(
                terms[2 * own_rows :]
            ).astype(jnp.float32)
            columns.append(
                both[:own_rows]
                + swap_across(both[own_rows:].astype(jnp.bfloat16)).astype(jnp.float32)
            )
        lowered = jnp.concatenate(columns, axis=1)
    else:
        partial_terms = jnp.dot(hidden, down_full, preferred_element_type=jnp.float32)
        lowered = lax.psum_scatter(
            partial_terms.astype(jnp.bfloat16), "tp", scatter_dimension=0, tiled=True
        ).astype(jnp.float32)
    lowered = lax.optimization_barrier(lowered.astype(jnp.bfloat16)).astype(jnp.float32)
    result = layer_norm(ALPHA * normed.astype(jnp.float32) + lowered, ffn_gain, ffn_bias)
    return result.astype(jnp.bfloat16)


def solution(mesh):
    placed = (
        P("sp", "tp"),
        P("sp", "tp"),
        P("sp", "tp"),
        P("sp", "tp"),
        P("sp", None),
        P("tp", None),
        P(),
        P(),
        P("sp", "tp"),
        P("sp", "tp"),
        P("tp", "sp"),
        P(),
        P(),
    )
    return jax.shard_map(
        body, mesh=mesh, in_specs=placed, out_specs=P(("sp", "tp"), None), check_vma=False
    )
```

```python
import jax
import jax.numpy as jnp
from jax import lax
from jax.experimental import pallas as pl
from jax.experimental.pallas import tpu as pltpu
from jax.sharding import PartitionSpec as P


ALPHA = 8.0**0.25
EPSILON = 1e-05


def layer_norm(matrix, norm_gain, norm_shift):
    centred = matrix - jnp.mean(matrix, axis=-1, keepdims=True)
    spread = jnp.mean(centred * centred, axis=-1, keepdims=True)
    return centred * lax.rsqrt(spread + EPSILON) * norm_gain + norm_shift


def attend(queries, key_rows, value_rows, log_forget):
    length, row_width = queries.shape
    head_count = log_forget.shape[1]
    head_dim = row_width // head_count
    score_scale = head_dim ** (-0.5)
    first_pos = lax.axis_index("sp") * length
    last_pos = first_pos + length
    query_heads = queries.reshape(length, head_count, head_dim)
    query_gates = log_forget.T
    query_pos = first_pos + jnp.arange(length, dtype=jnp.int32)
    gates_all = lax.all_gather(log_forget, "sp", axis=0, tiled=True)
    initial = (
        jnp.full((head_count, length), -1e30, jnp.float32),
        jnp.zeros((head_count, length), jnp.float32),
        jnp.zeros((length, head_count, head_dim), jnp.float32),
    )
    running = initial
    key_piece = lax.all_gather(key_rows, "sp", axis=0, tiled=True)
    value_piece = lax.all_gather(value_rows, "sp", axis=0, tiled=True)
    piece_len = key_piece.shape[0]
    shards = piece_len // length
    group_size = max(
        [
            count_try
            for count_try in range(1, shards + 1)
            if shards % count_try == 0 and count_try * length <= max(length, 512)
        ]
    )
    block_len = group_size * length
    blocks = piece_len // block_len
    key_blocks = key_piece.reshape(blocks, block_len, head_count, head_dim)
    value_blocks = value_piece.reshape(blocks, block_len, head_count, head_dim)
    gate_blocks = gates_all.reshape(blocks, block_len, head_count)
    block_starts = block_len * jnp.arange(blocks, dtype=jnp.int32)

    def one_block(running_state, packed):
        key_block, value_block, gate_block, block_start = packed

        def compute(state_in):
            highest, totals, weighted = state_in
            scores = (
                jnp.einsum(
                    "qhd,khd->hqk", query_heads, key_block, preferred_element_type=jnp.float32
                )
                * score_scale
            )
            scores = scores + query_gates[:, :, None] - gate_block.T[:, None, :]
            key_pos = block_start + jnp.arange(block_len, dtype=jnp.int32)
            allowed = (key_pos[None, :] <= query_pos[:, None])[None]
            masked = jnp.where(allowed, scores, -1e30)
            new_high = jnp.maximum(highest, jnp.max(masked, axis=2))
            weights = jnp.where(allowed, jnp.exp(masked - new_high[:, :, None]), 0.0)
            factor = jnp.exp(highest - new_high)
            totals = totals * factor + jnp.sum(weights, axis=2)
            weighted = weighted * factor.T[:, :, None] + jnp.einsum(
                "hqk,khd->qhd",
                weights.astype(jnp.bfloat16),
                value_block,
                preferred_element_type=jnp.float32,
            )
            return (new_high, totals, weighted)

        def keep_state(state_in):
            return state_in

        return (lax.cond(block_start < last_pos, compute, keep_state, running_state), None)

    running, unused = lax.scan(
        one_block, running, (key_blocks, value_blocks, gate_blocks, block_starts)
    )
    highest, totals, weighted = running
    return (weighted / totals.T[:, :, None]).reshape(length, row_width).astype(jnp.bfloat16)


SUB = 256


def flash_kernel(packed_ref, out_ref, query_ref, value_ref, high_ref, acc_ref):
    pieces, rows, length = packed_ref.shape
    head_dim = out_ref.shape[1]
    sub = SUB if length % SUB == 0 else length
    gate_rows = rows - 3 * head_dim
    query_at = head_dim + gate_rows
    value_at = query_at + head_dim
    tail = jnp.zeros((128 - head_dim - gate_rows, length), jnp.bfloat16)
    row_index = lax.broadcasted_iota(jnp.int32, (gate_rows, length), 0)
    minus = jnp.where(row_index < 3, -1.0, 0.0).astype(jnp.bfloat16)
    ones = jnp.where(row_index < 1, 1.0, 0.0).astype(jnp.bfloat16)
    scale = head_dim**-0.5

    def set_values(piece, carry):
        block = packed_ref[piece, value_at : value_at + head_dim, :]
        value_ref[piece] = jnp.concatenate([block, ones, tail], axis=0).T
        return carry

    lax.fori_loop(0, pieces, set_values, 0)

    def pair(piece, diagonal):
        key_block = packed_ref[piece, 0:128, :]
        for start in range(0, length, sub):
            width = min(length, start + sub) if diagonal else length
            keys = key_block[:, :width]
            scores = jnp.dot(
                query_ref[start : start + sub, :], keys, preferred_element_type=jnp.float32
            )
            if diagonal:
                key_pos = lax.broadcasted_iota(jnp.int32, (sub, width), 1)
                query_pos = start + lax.broadcasted_iota(jnp.int32, (sub, width), 0)
                scores = jnp.where(key_pos <= query_pos, scores, -1e30)
            old_high = high_ref[start : start + sub, :]
            new_high = jnp.maximum(old_high, jnp.max(scores, axis=1, keepdims=True))
            weights = jnp.exp(scores - new_high[:, :1]).astype(jnp.bfloat16)
            factor = jnp.exp(old_high - new_high)
            high_ref[start : start + sub, :] = new_high
            acc_ref[start : start + sub, :] = acc_ref[start : start + sub, :] * factor + jnp.dot(
                weights, value_ref[piece, :width, :], preferred_element_type=jnp.float32
            )

    def one_query_piece(index, carry):
        block = packed_ref[index, query_at : query_at + head_dim, :]
        scaled = (block.astype(jnp.float32) * scale).astype(jnp.bfloat16)
        query_ref[...] = jnp.concatenate([scaled, minus, tail], axis=0).T
        high_ref[...] = jnp.full_like(high_ref, -1e30)
        acc_ref[...] = jnp.zeros_like(acc_ref)

        def earlier(piece, inner):
            pair(piece, False)
            return inner

        lax.fori_loop(0, index, earlier, 0)
        pair(index, True)
        turned = acc_ref[...].T
        out_ref[index] = (turned[:head_dim] / turned[head_dim : head_dim + 1]).astype(jnp.bfloat16)
        return carry

    lax.fori_loop(0, pieces, one_query_piece, 0)


def attend_by_head(queries, key_rows, value_rows, log_forget):
    length, row_width = queries.shape
    heads = log_forget.shape[1]
    head_dim = row_width // heads
    pieces = lax.axis_size("sp")

    def turn(matrix):
        return matrix.T.reshape(heads, head_dim, length)

    gates = log_forget.T
    high = lax.reduce_precision(gates, 8, 7)
    middle = lax.reduce_precision(gates - high, 8, 7)
    low = gates - high - middle
    gate_rows = jnp.stack([high, middle, low], axis=1).astype(jnp.bfloat16)
    gate_rows = jnp.pad(gate_rows, ((0, 0), (0, 13), (0, 0)))
    packed = jnp.concatenate(
        [turn(key_rows), gate_rows, turn(queries), turn(value_rows)], axis=1
    )
    packed = lax.all_to_all(packed, "sp", 0, 0, tiled=True)
    flops = 2 * pieces * pieces * length * length * 128
    attended = pl.pallas_call(
        flash_kernel,
        out_shape=jax.ShapeDtypeStruct((pieces, head_dim, length), jnp.bfloat16),
        in_specs=[pl.BlockSpec(memory_space=pltpu.VMEM)],
        out_specs=pl.BlockSpec(memory_space=pltpu.VMEM),
        scratch_shapes=[
            pltpu.VMEM((length, 128), jnp.bfloat16),
            pltpu.VMEM((pieces, length, 128), jnp.bfloat16),
            pltpu.VMEM((length, 128), jnp.float32),
            pltpu.VMEM((length, 128), jnp.float32),
        ],
        compiler_params=pltpu.CompilerParams(vmem_limit_bytes=40 * 1024 * 1024),
        cost_estimate=pl.CostEstimate(
            flops=4 * flops, bytes_accessed=packed.size * 2, transcendentals=0
        ),
    )(packed)
    back = lax.all_to_all(attended, "sp", 0, 0, tiled=True)
    return back.reshape(row_width, length)


def swap_cores(block):
    count = lax.axis_size("tp")
    return lax.ppermute(block, "tp", [(i, i ^ 1) for i in range(count)])


def swap_across(block):
    count = lax.axis_size("tp")
    return lax.ppermute(block, "tp", [(i, i ^ 2) for i in range(count)])


def body(
    queries,
    key_rows,
    value_rows,
    log_forget,
    stream_in,
    out_weight,
    mix_gain,
    mix_bias,
    gate_weight,
    up_weight,
    down_weight,
    ffn_gain,
    ffn_bias,
):
    gate_full = lax.all_gather(gate_weight, "sp", axis=0, tiled=True)
    up_full = lax.all_gather(up_weight, "sp", axis=0, tiled=True)
    shards = lax.axis_size("sp")
    narrow = down_weight.shape[1] // 2
    halved = lax.axis_size("tp") == 4 and narrow % 128 == 0
    if halved:
        down_parts = [
            lax.all_gather(down_weight[:, start : start + narrow], "sp", axis=1, tiled=True)
            for start in (0, narrow)
        ]
    else:
        down_full = lax.all_gather(down_weight, "sp", axis=1, tiled=True)
    length = queries.shape[0]
    heads = log_forget.shape[1]
    head_dim = queries.shape[1] // heads
    by_head = heads == lax.axis_size("sp") and head_dim + 16 <= 128 and head_dim % 16 == 0
    if by_head:
        turned = attend_by_head(queries, key_rows, value_rows, log_forget)
    else:
        turned = attend(queries, key_rows, value_rows, log_forget).T
    own_rows = length // lax.axis_size("tp")
    offset = lax.axis_index("tp") * own_rows
    two_level = halved
    partial_mix = lax.dot_general(
        turned, out_weight, (((0,), (0,)), ((), ())), preferred_element_type=jnp.float32
    ).astype(jnp.bfloat16)
    if two_level:
        core = lax.axis_index("tp") % 2
        across = lax.axis_index("tp") // 2
        split = partial_mix.reshape(2, 2, own_rows, -1)
        mine = lax.dynamic_index_in_dim(split, core, 1, keepdims=False)
        other = lax.dynamic_index_in_dim(split, 1 - core, 1, keepdims=False)
        both = mine.astype(jnp.float32) + swap_cores(other).astype(jnp.float32)
        own = lax.dynamic_index_in_dim(both, across, 0, keepdims=False)
        away = lax.dynamic_index_in_dim(both, 1 - across, 0, keepdims=False)
        summed = (own + swap_across(away.astype(jnp.bfloat16)).astype(jnp.float32)).astype(
            jnp.bfloat16
        )
    else:
        summed = lax.psum_scatter(partial_mix, "tp", scatter_dimension=0, tiled=True)
    mix_out = lax.optimization_barrier(summed).astype(jnp.float32)
    stream_own = lax.dynamic_slice_in_dim(stream_in, offset, own_rows, 0)
    normed = layer_norm(
        ALPHA * stream_own.astype(jnp.float32) + mix_out, mix_gain, mix_bias
    ).astype(jnp.bfloat16)
    if two_level:
        pair = jnp.concatenate([normed, swap_across(normed)], axis=0)
        gathered = jnp.concatenate([pair, swap_cores(pair)], axis=0)
    else:
        gathered = lax.all_gather(normed, "tp", axis=0, tiled=True)
    gate_part = jnp.dot(gathered, gate_full, preferred_element_type=jnp.float32)
    up_part = jnp.dot(gathered, up_full, preferred_element_type=jnp.float32)
    hidden = (jax.nn.silu(gate_part) * up_part).astype(jnp.bfloat16)
    if two_level:
        columns = []
        for down_part in down_parts:
            terms = jnp.dot(hidden, down_part, preferred_element_type=jnp.float32).astype(
                jnp.bfloat16
            )
            both = terms[: 2 * own_rows].astype(jnp.float32) + swap_cores(
                terms[2 * own_rows :]
            ).astype(jnp.float32)
            away, hidden = lax.optimization_barrier((both[own_rows:].astype(jnp.bfloat16), hidden))
            columns.append(both[:own_rows] + swap_across(away).astype(jnp.float32))
        lowered = jnp.concatenate(
            [
                column[:, piece * narrow : (piece + 1) * narrow]
                for piece in range(shards)
                for column in columns
            ],
            axis=1,
        )
    else:
        partial_terms = jnp.dot(hidden, down_full, preferred_element_type=jnp.float32)
        lowered = lax.psum_scatter(
            partial_terms.astype(jnp.bfloat16), "tp", scatter_dimension=0, tiled=True
        ).astype(jnp.float32)
    lowered = lax.optimization_barrier(lowered.astype(jnp.bfloat16)).astype(jnp.float32)
    result = layer_norm(ALPHA * normed.astype(jnp.float32) + lowered, ffn_gain, ffn_bias)
    return result.astype(jnp.bfloat16)


def solution(mesh):
    placed = (
        P("sp", "tp"),
        P("sp", "tp"),
        P("sp", "tp"),
        P("sp", "tp"),
        P("sp", None),
        P("tp", None),
        P(),
        P(),
        P("sp", "tp"),
        P("sp", "tp"),
        P("tp", "sp"),
        P(),
        P(),
    )
    return jax.shard_map(
        body, mesh=mesh, in_specs=placed, out_specs=P(("sp", "tp"), None), check_vma=False
    )
```
